32 devices in a mesh: sp: 16 (over z, y, x), tp: 2 (over core).
Axes of the slice: x: 2, y: 2, z: 4, core: 2. Of those that a mesh axis runs over, the one named last changes fastest.
Arguments:
- queries: bfloat16 [1, 6144, 2048], P(None, 'sp', 'tp'), may hold values from -5 to 5
- keys: bfloat16 [1, 6144, 2048], P(None, 'sp', 'tp'), may hold values from -5 to 5
- values: bfloat16 [1, 6144, 2048], P(None, 'sp', 'tp'), may hold values from -6 to 6
- rel_bias: float32 [16, 192], P('tp'), may hold values from -3 to 3
- out_grad: bfloat16 [1, 6144, 2048], P(None, 'sp', 'tp'), may hold values from -48 to 48
Outputs:
- query_grad: bfloat16 [1, 6144, 2048], P(None, 'sp', 'tp')
- key_grad: bfloat16 [1, 6144, 2048], P(None, 'sp', 'tp')
- value_grad: bfloat16 [1, 6144, 2048], P(None, 'sp', 'tp')
- bias_grad: float32 [16, 192], replicated
The draws below stay inside these ranges and needn't reach their ends.
All inputs are finite; a program needn't handle non-finite values.
Results may differ from the reference program's by a relative error of at most 0.0049.
Values may be sent and summed in bfloat16 or wider, within the bound.
A program may use at most 64 MiB of HBM per device.

```python
import jax
import jax.numpy as jnp
from jax import lax

HEADS = 16
HEAD_DIM = 128
SEG = 64
LEFT = 4
CLIP = 128
SEQS = 1
TOK_DEV = 384
LENGTH = 6144
WIDTH = 2048
BAND = 320
BUCKETS = 192


def aligned_pair(key):
    shape = (SEQS, LENGTH, HEADS * HEAD_DIM)
    base_q = jax.random.normal(jax.random.fold_in(key, 11), shape, jnp.float32)
    base_k = jax.random.normal(jax.random.fold_in(key, 12), shape, jnp.float32)
    return (jnp.clip(base_q, -5.0, 5.0), jnp.clip(base_k, -5.0, 5.0))


def draw_queries(key, part):
    return aligned_pair(key)[0].astype(jnp.bfloat16)


def draw_keys(key, part):
    return aligned_pair(key)[1].astype(jnp.bfloat16)


def steps_of(own_key, dims, pieces, smallest, high):
    def one(dim, blocks):
        heights = jax.random.uniform(jax.random.fold_in(jax.random.fold_in(own_key, 6), dim), (blocks,), jnp.float32, smallest / len(pieces), high / len(pieces))
        return jnp.repeat(jnp.exp(heights), dims[dim] // blocks).reshape((-1,) + (1,) * (len(dims) - dim - 1))

    gain = one(*pieces[0])
    for cut in pieces[1:]:
        gain = gain * one(*cut)
    return gain


def gaussian(rng, shape, width, limit, shards=(), held_as=jnp.bfloat16):
    factor_of = steps_of(rng, shape, shards, -0.22, 0.18) if shards else 1.0
    drawn = jax.random.normal(rng, shape, jnp.float32) * width * factor_of
    return jnp.minimum(jnp.maximum(drawn, -limit), limit).astype(held_as)


def setup_inputs(seed: int = 0) -> dict:
    arg_keys = jax.random.split(jax.random.key(seed), 6)
    queries = draw_queries(jax.random.fold_in(arg_keys[5], 71), 0)
    keys = draw_keys(jax.random.fold_in(arg_keys[5], 71), 0)
    values = gaussian(arg_keys[2], (SEQS, LENGTH, WIDTH), 1.0, 6.0, ((1, 16), (2, 2)))
    rel_bias = gaussian(arg_keys[3], (HEADS, BUCKETS), 0.5, 3.0, ((0, 2),), jnp.float32)
    out_grad = gaussian(arg_keys[4], (SEQS, LENGTH, WIDTH), 8.0, 48.0, ((1, 16), (2, 2)))
    return dict(queries=queries, keys=keys, values=values, rel_bias=rel_bias, out_grad=out_grad)


def relative_index():
    rows = jnp.arange(SEG, dtype=jnp.int32)[:, None] + LEFT * SEG
    cols = jnp.arange(BAND, dtype=jnp.int32)[None, :]
    return (jnp.clip(rows - cols, 1 - SEG, CLIP) + SEG - 1).astype(jnp.int32)


def low_round(array):
    return lax.optimization_barrier(array.astype(jnp.bfloat16)).astype(jnp.float32)


def band_math(q_segs, k_band, v_band, g_segs, table, key_valid):
    seg_count = q_segs.shape[1]
    score_scale = HEAD_DIM ** -0.5
    q_full = q_segs.astype(jnp.float32)
    g_full = g_segs.astype(jnp.float32)
    k_full = k_band.astype(jnp.float32)
    v_full = v_band.astype(jnp.float32)
    score_parts = []
    prob_parts = []
    for offset in range(LEFT + 1):
        score_parts.append(jnp.einsum('sncha,snkha->snhck', q_full, k_full[:, offset:offset + seg_count]))
        prob_parts.append(jnp.einsum('sncha,snkha->snhck', g_full, v_full[:, offset:offset + seg_count]))
    score = jnp.concatenate(score_parts, axis=-1) * score_scale + table[None, None]
    score = jnp.where(key_valid[None, :, None, None, :], score, -jnp.inf)
    row_max = jnp.max(score, axis=-1, keepdims=True)
    expo = jnp.exp(score - row_max)
    prob = expo / jnp.sum(expo, axis=-1, keepdims=True)
    prob_grad = jnp.concatenate(prob_parts, axis=-1)
    row_delta = jnp.sum(prob * prob_grad, axis=-1, keepdims=True)
    score_grad = prob * (prob_grad - row_delta)
    bias_terms = jnp.sum(score_grad, axis=(0, 1))
    prob_low = low_round(prob)
    grad_low = low_round(score_grad * score_scale)
    query_acc = jnp.zeros(q_full.shape, jnp.float32)
    key_acc = jnp.zeros(k_full.shape, jnp.float32)
    value_acc = jnp.zeros(k_full.shape, jnp.float32)
    for offset in range(LEFT + 1):
        grad_part = grad_low[..., offset * SEG:(offset + 1) * SEG]
        prob_part = prob_low[..., offset * SEG:(offset + 1) * SEG]
        query_acc = query_acc + jnp.einsum('snhck,snkha->sncha', grad_part, k_full[:, offset:offset + seg_count])
        key_acc = key_acc.at[:, offset:offset + seg_count].add(jnp.einsum('snhck,sncha->snkha', grad_part, q_full))
        value_acc = value_acc.at[:, offset:offset + seg_count].add(jnp.einsum('snhck,sncha->snkha', prob_part, g_full))
    return query_acc, key_acc, value_acc, bias_terms


def reference(queries, keys, values, rel_bias, out_grad):
    seq_count, length, row_width = queries.shape
    head_count = row_width // HEAD_DIM
    reach = LEFT * SEG
    block_rows = TOK_DEV
    seg_count = block_rows // SEG
    zero_rows = jnp.zeros((seq_count, reach, row_width), keys.dtype)
    keys_pad = jnp.concatenate([zero_rows, keys], axis=1)
    values_pad = jnp.concatenate([zero_rows, values], axis=1)
    rel_ids = relative_index()
    table = jnp.take(rel_bias.astype(jnp.float32), rel_ids, axis=1)
    seg_shape = (seq_count, seg_count, SEG, head_count, HEAD_DIM)
    band_shape = (seq_count, seg_count + LEFT, SEG, head_count, HEAD_DIM)

    def step(carry, block):
        key_sum, value_sum, bias_sum = carry
        start = (block * block_rows).astype(jnp.int32)
        q_blk = lax.dynamic_slice_in_dim(queries, start, block_rows, 1).reshape(seg_shape)
        g_blk = lax.dynamic_slice_in_dim(out_grad, start, block_rows, 1).reshape(seg_shape)
        k_blk = lax.dynamic_slice_in_dim(keys_pad, start, block_rows + reach, 1).reshape(band_shape)
        v_blk = lax.dynamic_slice_in_dim(values_pad, start, block_rows + reach, 1).reshape(band_shape)
        positions = start + jnp.arange(seg_count, dtype=jnp.int32)[:, None] * SEG - reach + jnp.arange(BAND, dtype=jnp.int32)[None, :]
        key_valid = positions >= 0
        query_acc, key_acc, value_acc, bias_terms = band_math(q_blk, k_blk, v_blk, g_blk, table, key_valid)
        flat = (seq_count, block_rows + reach, row_width)
        key_sum = lax.dynamic_update_slice_in_dim(key_sum, lax.dynamic_slice_in_dim(key_sum, start, block_rows + reach, 1) + key_acc.reshape(flat), start, 1)
        value_sum = lax.dynamic_update_slice_in_dim(value_sum, lax.dynamic_slice_in_dim(value_sum, start, block_rows + reach, 1) + value_acc.reshape(flat), start, 1)
        query_out = query_acc.astype(jnp.bfloat16).reshape(seq_count, block_rows, row_width)
        return (key_sum, value_sum, bias_sum + bias_terms), query_out

    init = (jnp.zeros((seq_count, length + reach, row_width), jnp.float32),
            jnp.zeros((seq_count, length + reach, row_width), jnp.float32),
            jnp.zeros((head_count, SEG, BAND), jnp.float32))
    (key_sum, value_sum, bias_sum), query_blocks = lax.scan(step, init, jnp.arange(length // block_rows, dtype=jnp.int32))
    query_grad = jnp.transpose(query_blocks, (1, 0, 2, 3)).reshape(seq_count, length, row_width)
    key_grad = key_sum[:, reach:].astype(jnp.bfloat16)
    value_grad = value_sum[:, reach:].astype(jnp.bfloat16)
    bias_grad = jax.ops.segment_sum(bias_sum.reshape(head_count, -1).T, rel_ids.reshape(-1), num_segments=BUCKETS).T
    return query_grad, key_grad, value_grad, bias_grad
```

```python
import functools

import jax
import jax.numpy as jnp
from jax import lax
from jax.experimental import pallas as pl
from jax.experimental.pallas import tpu as pltpu
from jax.sharding import PartitionSpec as P

HEAD_DIM = 128
SEG = 64
LEFT = 4
BUCKETS = 192
TILE = 2 * SEG
REACH = LEFT * SEG
SPAN = REACH + TILE
LANES = 256
LOW = -1e30
SCALE = HEAD_DIM ** (-0.5)
MESH = pl.DeviceIdType.MESH
F32 = jnp.float32
BF16 = jnp.bfloat16

NT = (((1,), (1,)), ((), ()))
TN = (((0,), (0,)), ((), ()))
NN = (((1,), (0,)), ((), ()))


def dot(a, b, dims):
    return lax.dot_general(a, b, dims, preferred_element_type=F32)


def toeplitz(row):
    x = jnp.broadcast_to(row, (8, LANES))
    x = pltpu.roll(x, LANES - (SEG - 1), axis=1)
    sub = lax.broadcasted_iota(jnp.int32, (8, LANES), 0)
    for bit in (1, 2, 4):
        x = jnp.where((sub & bit) != 0, pltpu.roll(x, bit, axis=1), x)
    rows = 8
    while rows < TILE:
        x = jnp.concatenate([x, pltpu.roll(x, rows, axis=1)], axis=0)
        rows *= 2
    return x


def skew_sum(z):
    rows = TILE
    while rows > 8:
        half = rows // 2
        z = z[:half] + pltpu.roll(z[half:], LANES - half, axis=1)
        rows = half
    for half in (4, 2, 1):
        z = z + pltpu.roll(pltpu.roll(z, 8 - half, axis=0), LANES - half, axis=1)
    return pltpu.roll(z, SEG - 1, axis=1)[0:1]


def partial_stats(s, dp):
    m = jnp.max(s, axis=0, keepdims=True)
    e = jnp.exp(s - m)
    return e, m, jnp.sum(e, axis=0, keepdims=True), jnp.sum(e * dp, axis=0, keepdims=True)


def merged(e, dp, mine, other):
    m, l, d = mine
    mo, lo, do = other
    top = jnp.maximum(m, mo)
    c, co = jnp.exp(m - top), jnp.exp(mo - top)
    inv = 1.0 / (l * c + lo * co)
    delta = (d * c + do * co) * inv
    p = e * (c * inv)
    return p, p * (dp - delta)


def pack(a, b):
    zero = jnp.zeros((2, TILE), F32)
    return jnp.concatenate([*a, *b, zero], axis=0)


def unpack(st):
    rows = [st[i : i + 1] for i in range(6)]
    return rows[:3], rows[3:]


def kernel(
    sp_n, tp_n, low_n, heads, tok,
    q_hbm, k_hbm, v_hbm, g_hbm, rb_ref,
    dq_hbm, dk_hbm, dv_hbm, bias_ref,
    q, k, v, g, dqo, dko, dvo, rq, rg, rbp, table, gsum, acck, accv, es, dps,
    st_own, st_next, st_half, st_prev, dq_loc, dq_out, dq_in,
    b0, b1, b2, slots1, slots2, slots3,
    in_sem, q_s, q_r, g_s, g_r, so_s, so_r, sh_s, sh_r, dq_s, dq_r,
    e1_s, e1_r, e2_s, e2_r, e3_s, e3_r, kv_sem, dqo_sem,
):
    sp = lax.axis_index("sp")
    tp = lax.axis_index("tp")
    high_n = sp_n // low_n
    low, high = lax.rem(sp, low_n), lax.div(sp, low_n)
    has_prev = sp > 0
    has_next = sp < sp_n - 1
    groups = tok // TILE
    lead = min(3, heads)
    half_heads = heads // 2

    def cols_of(h):
        return pl.ds(pl.multiple_of(h * HEAD_DIM, HEAD_DIM), HEAD_DIM)

    loads = [
        pltpu.make_async_copy(src.at[0], dst, in_sem.at[i])
        for i, (src, dst) in enumerate(((q_hbm, q), (k_hbm, k), (g_hbm, g), (v_hbm, v)))
    ]
    for load in loads:
        load.start()

    barrier = pltpu.get_barrier_semaphore()

    def greet(axis, index):
        pl.semaphore_signal(barrier, inc=1, device_id={axis: index}, device_id_type=MESH)

    @pl.when(has_prev)
    def _():
        greet("sp", sp - 1)

    @pl.when(has_next)
    def _():
        greet("sp", sp + 1)

    for d in range(1, low_n):
        greet("sp", high * low_n + lax.rem(low + d, low_n))
    for d in range(1, high_n):
        greet("sp", lax.rem(high + d, high_n) * low_n + low)
    for d in range(1, tp_n):
        greet("tp", lax.rem(tp + d, tp_n))
    ends = (sp == 0).astype(jnp.int32) + (sp == sp_n - 1).astype(jnp.int32)
    pl.semaphore_wait(barrier, low_n + high_n + tp_n - 1 - ends)

    def q_copy(h):
        return pltpu.make_async_remote_copy(
            q_hbm.at[0, pl.ds(0, REACH), cols_of(h)], rq.at[h], q_s.at[h], q_r.at[h],
            device_id={"sp": sp - 1}, device_id_type=MESH)

    def g_copy(h):
        return pltpu.make_async_remote_copy(
            g_hbm.at[0, pl.ds(0, REACH), cols_of(h)], rg.at[h], g_s.at[h], g_r.at[h],
            device_id={"sp": sp - 1}, device_id_type=MESH)

    own_copy = pltpu.make_async_remote_copy(
        st_own, st_next, so_s.at[0], so_r.at[0], device_id={"sp": sp - 1}, device_id_type=MESH)

    def half_copy(h):
        return pltpu.make_async_remote_copy(
            st_half.at[h], st_prev.at[h], sh_s.at[h], sh_r.at[h],
            device_id={"sp": sp + 1}, device_id_type=MESH)

    def dq_copy(h):
        return pltpu.make_async_remote_copy(
            dq_out.at[h], dq_in.at[h], dq_s.at[h], dq_r.at[h],
            device_id={"sp": sp + 1}, device_id_type=MESH)

    @pl.when(has_prev)
    def _():
        @pl.loop(0, lead)
        def _(h):
            q_copy(h).start()
            g_copy(h).start()

    row_b = lax.broadcasted_iota(jnp.int32, (TILE, TILE), 0)
    col_r = lax.broadcasted_iota(jnp.int32, (TILE, TILE), 1)
    far_ok = (col_r < SEG) | (row_b >= SEG)
    diag_ok = (row_b < SEG) | (col_r >= SEG)
    beyond = col_r >= row_b
    lane = lax.broadcasted_iota(jnp.int32, (1, LANES), 1)

    rbp[...] = jnp.zeros_like(rbp)
    rbp[0:heads, 0:BUCKETS] = rb_ref[...]
    b0[...] = jnp.zeros_like(b0)

    for load in loads:
        load.wait()

    @pl.loop(0, heads)
    def _(h):
        cols = cols_of(h)
        row = rbp[pl.ds(h, 1), :]
        last = jnp.sum(jnp.where(lane == BUCKETS - 1, row, 0.0), axis=1, keepdims=True)
        both = toeplitz(row)
        far = jnp.where(far_ok, jnp.broadcast_to(last, (TILE, TILE)), LOW)
        mid = jnp.where(beyond, jnp.broadcast_to(last, (TILE, TILE)), both[:, TILE:])
        diag = jnp.where(diag_ok, both[:, :TILE], LOW)
        tab = jnp.concatenate([far, mid, diag], axis=0)
        table[h] = tab

        def tiles(group, keys_from, tab_part):
            size = tab_part.shape[0]
            rows = slice(group * TILE, (group + 1) * TILE)
            keys = slice(keys_from, keys_from + size)
            s = dot(k[keys, cols], q[rows, cols], NT) * SCALE + tab_part
            dp = dot(v[keys, cols], g[rows, cols], NT)
            return s, dp

        s, dp = tiles(0, 0, diag)
        e0, *st0 = partial_stats(s, dp)
        es[h, 0:TILE] = e0
        dps[h, 0:TILE] = dp
        s, dp = tiles(1, 0, tab[TILE:])
        e1, *st1 = partial_stats(s, dp)
        es[h, TILE:SPAN] = e1
        dps[h, TILE:SPAN] = dp
        st_own[h] = pack(st0, st1)

        for group in range(2, groups):
            start = (group - 2) * TILE
            rows = slice(group * TILE, (group + 1) * TILE)
            keys = slice(start, start + SPAN)
            s, dp = tiles(group, start, tab)
            e, m, l, d = partial_stats(s, dp)
            inv = 1.0 / l
            p = e * inv
            sg = p * (dp - d * inv)
            low_p = p.astype(BF16)
            low_g = (sg * SCALE).astype(BF16)
            part_k = dot(low_g, q[rows, cols], NN)
            part_v = dot(low_p, g[rows, cols], NN)
            if group == 2:
                gsum[h] = sg
                acck[h, 0:SPAN] = part_k
                accv[h, 0:SPAN] = part_v
            else:
                gsum[h] += sg
                old = slice(start, start + REACH)
                new = slice(start + REACH, start + SPAN)
                acck[h, old] += part_k[:REACH]
                accv[h, old] += part_v[:REACH]
                acck[h, new] = part_k[REACH:]
                accv[h, new] = part_v[REACH:]
            dqo[rows, cols] = dot(low_g, k[keys, cols], TN).astype(BF16)

    @pl.when(has_prev)
    def _():
        own_copy.start()
        if lead < heads:
            @pl.loop(lead, heads)
            def _(h):
                q_copy(h).start()
                g_copy(h).start()

    @pl.when(jnp.logical_not(has_prev))
    def _():
        none = [jnp.full((1, TILE), LOW, F32), jnp.zeros((1, TILE), F32), jnp.zeros((1, TILE), F32)]
        nothing = pack(none, none)

        @pl.loop(0, heads)
        def _(h):
            st_prev[h] = nothing
            dq_in[h] = jnp.zeros((REACH, HEAD_DIM), BF16)

    @pl.when(has_next)
    def _():
        own_copy.wait_recv()

        @pl.loop(0, heads)
        def _(h):
            cols = cols_of(h)
            q_copy(h).wait_recv()
            g_copy(h).wait_recv()
            other0, other1 = unpack(st_next[h])

            def side(rows, keys_from, size, other):
                keys = slice(keys_from, keys_from + size)
                qr, gr = rq[h, rows], rg[h, rows]
                s = dot(k[keys, cols], qr, NT) * SCALE + table[h, 0:size]
                dp = dot(v[keys, cols], gr, NT)
                e, *mine = partial_stats(s, dp)
                p, sg = merged(e, dp, mine, other)
                gsum[h, 0:size] += sg
                low_p = p.astype(BF16)
                low_g = (sg * SCALE).astype(BF16)
                acck[h, keys] += dot(low_g, qr, NN)
                accv[h, keys] += dot(low_p, gr, NN)
                dq_out[h, rows] = dot(low_g, k[keys, cols], TN).astype(BF16)
                return mine

            mine0 = side(slice(0, TILE), tok - REACH, REACH, other0)
            mine1 = side(slice(TILE, REACH), tok - TILE, TILE, other1)
            st_half[h] = pack(mine0, mine1)
            half_copy(h).start()

        @pl.loop(0, half_heads)
        def _(h):
            dq_copy(h).start()

    @pl.loop(0, heads)
    def _(h):
        cols = cols_of(h)

        @pl.when(has_prev)
        def _():
            half_copy(h).wait_recv()

        other0, other1 = unpack(st_prev[h])
        mine0, mine1 = unpack(st_own[h])
        p0, sg0 = merged(es[h, 0:TILE], dps[h, 0:TILE], mine0, other0)
        p1, sg1 = merged(es[h, TILE:SPAN], dps[h, TILE:SPAN], mine1, other1)
        sums = gsum[h]
        far = sums[:TILE]
        mid = sums[TILE:REACH] + sg1[:TILE]
        diag = sums[REACH:] + sg1[TILE:] + sg0
        clipped = jnp.sum(far + jnp.where(beyond, mid, 0.0), axis=0, keepdims=True)
        clipped = jnp.sum(clipped, axis=1, keepdims=True)
        both = jnp.concatenate([diag, jnp.where(beyond, 0.0, mid)], axis=1)
        b0[pl.ds(h, 1), :] = skew_sum(both) + jnp.where(lane == BUCKETS - 1, clipped, 0.0)

        gl0, gl1 = (sg0 * SCALE).astype(BF16), (sg1 * SCALE).astype(BF16)
        q0, q1 = q[0:TILE, cols], q[TILE:REACH, cols]
        g0, g1 = g[0:TILE, cols], g[TILE:REACH, cols]
        for acc, out, a0, a1, x0, x1 in (
            (acck, dko, gl0, gl1, q0, q1), (accv, dvo, p0.astype(BF16), p1.astype(BF16), g0, g1)):
            second = dot(a1, x1, NN)
            out[0:TILE, cols] = (acc[h, 0:TILE] + second[:TILE] + dot(a0, x0, NN)).astype(BF16)
            out[TILE:REACH, cols] = (acc[h, TILE:REACH] + second[TILE:]).astype(BF16)
            out[REACH:tok, cols] = acc[h, REACH:tok].astype(BF16)
        dq_loc[h, 0:TILE] = dot(gl0, k[0:TILE, cols], TN)
        dq_loc[h, TILE:REACH] = dot(gl1, k[0:REACH, cols], TN)

    dk_store = pltpu.make_async_copy(dko, dk_hbm.at[0], kv_sem.at[0])
    dv_store = pltpu.make_async_copy(dvo, dv_hbm.at[0], kv_sem.at[1])

    def copies(src, slots, send, recv, index, count, device):
        outgoing, incoming = [], []
        for d in range(1, count):
            peer = lax.rem(index + d, count)
            outgoing.append(pltpu.make_async_remote_copy(
                src, slots.at[index], send.at[d - 1], recv.at[index],
                device_id=device(peer), device_id_type=MESH))
            incoming.append(pltpu.make_async_remote_copy(
                src, slots.at[peer], send.at[d - 1], recv.at[peer],
                device_id=device(peer), device_id_type=MESH))
        return outgoing, incoming

    out1, in1 = copies(b0, slots1, e1_s, e1_r, low, low_n, lambda p: {"sp": high * low_n + p})
    out2, in2 = copies(b1, slots2, e2_s, e2_r, high, high_n, lambda p: {"sp": p * low_n + low})
    out3, in3 = copies(b2, slots3, e3_s, e3_r, tp, tp_n, lambda p: {"tp": p})

    for copy in out1:
        copy.start()
    slots1[low] = b0[...]
    dk_store.start()
    dv_store.start()

    @pl.when(has_next)
    def _():
        @pl.loop(half_heads, heads - 1)
        def _(h):
            dq_copy(h).start()

    for copy in in1:
        copy.wait_recv()
    total = slots1[0]
    for i in range(1, low_n):
        total += slots1[i]
    b1[...] = total
    for copy in out2:
        copy.start()
    slots2[high] = total

    @pl.when(has_next)
    def _():
        dq_copy(heads - 1).start()

    for copy in in2:
        copy.wait_recv()
    total = slots2[0]
    for i in range(1, high_n):
        total += slots2[i]
    b2[...] = total
    for copy in out3:
        copy.start()
    slots3[tp] = total

    def dq_store(h):
        cols = cols_of(h)
        return pltpu.make_async_copy(dqo.at[:, cols], dq_hbm.at[0, :, cols], dqo_sem.at[h])

    @pl.loop(0, heads)
    def _(h):
        @pl.when(has_prev)
        def _():
            dq_copy(h).wait_recv()

        dqo[0:REACH, cols_of(h)] = (dq_loc[h] + dq_in[h].astype(F32)).astype(BF16)
        dq_store(h).start()

    for copy in in3:
        copy.wait_recv()
    for i in range(tp_n):
        bias_ref[i * heads : (i + 1) * heads, :] = slots3[i, 0:heads, 0:BUCKETS]

    for copy in out1 + out2 + out3:
        copy.wait_send()

    @pl.when(has_prev)
    def _():
        own_copy.wait_send()

        @pl.loop(0, heads)
        def _(h):
            q_copy(h).wait_send()
            g_copy(h).wait_send()

    @pl.when(has_next)
    def _():
        @pl.loop(0, heads)
        def _(h):
            half_copy(h).wait_send()
            dq_copy(h).wait_send()

    dk_store.wait()
    dv_store.wait()

    @pl.loop(0, heads)
    def _(h):
        dq_store(h).wait()


def local(sp_n, tp_n, queries, keys, values, rel_bias, out_grad):
    seq_count, tok, width = queries.shape
    heads = width // HEAD_DIM
    low_n = max(d for d in range(1, sp_n + 1) if sp_n % d == 0 and d * d <= sp_n)
    high_n = sp_n // low_n
    pad = -(-heads // 8) * 8
    any_spec = pl.BlockSpec(memory_space=pl.ANY)
    vmem_spec = pl.BlockSpec(memory_space=pltpu.VMEM)
    block = jax.ShapeDtypeStruct(queries.shape, BF16)
    dma = pltpu.SemaphoreType.DMA
    big = pltpu.VMEM((tok, width), BF16)
    span = pltpu.VMEM((heads, SPAN, TILE), F32)
    acc = pltpu.VMEM((heads, tok, HEAD_DIM), F32)
    stats = pltpu.VMEM((heads, 8, TILE), F32)
    halo = pltpu.VMEM((heads, REACH, HEAD_DIM), BF16)
    row = pltpu.VMEM((pad, LANES), F32)
    return pl.pallas_call(
        functools.partial(kernel, sp_n, tp_n, low_n, heads, tok),
        out_shape=(block, block, block, jax.ShapeDtypeStruct((heads * tp_n, BUCKETS), F32)),
        in_specs=[any_spec] * 4 + [vmem_spec],
        out_specs=(any_spec, any_spec, any_spec, vmem_spec),
        scratch_shapes=[big] * 7 + [halo, halo, row, span, span, acc, acc, span, span]
        + [stats] * 4
        + [pltpu.VMEM((heads, REACH, HEAD_DIM), F32), halo, halo]
        + [row, row, row]
        + [pltpu.VMEM((n, pad, LANES), F32) for n in (low_n, high_n, tp_n)]
        + [dma((4,))] + [dma((heads,))] * 4 + [dma((1,))] * 2 + [dma((heads,))] * 4
        + [dma((low_n,))] * 2 + [dma((high_n,))] * 2 + [dma((tp_n,))] * 2
        + [dma((2,)), dma((heads,))],
        compiler_params=pltpu.CompilerParams(
            collective_id=0, has_side_effects=True, vmem_limit_bytes=56 * 1024 * 1024
        ),
    )(queries, keys, values, out_grad, rel_bias)


def solution(mesh):
    split = P(None, "sp", "tp")
    return jax.shard_map(
        functools.partial(local, mesh.shape["sp"], mesh.shape["tp"]),
        mesh=mesh,
        in_specs=(split, split, split, P("tp", None), split),
        out_specs=(split, split, split, P()),
        check_vma=False,
    )
```

```python
import functools

import jax
import jax.numpy as jnp
from jax import lax
from jax.experimental import pallas as pl
from jax.experimental.pallas import tpu as pltpu
from jax.sharding import PartitionSpec as P

HEAD_DIM = 128
SEG = 64
LEFT = 4
BUCKETS = 192
TILE = 2 * SEG
REACH = LEFT * SEG
SPAN = REACH + TILE
LANES = 256
LOW = -1e30
SCALE = HEAD_DIM ** (-0.5)
MESH = pl.DeviceIdType.MESH
F32 = jnp.float32
BF16 = jnp.bfloat16

NT = (((1,), (1,)), ((), ()))
TN = (((0,), (0,)), ((), ()))
NN = (((1,), (0,)), ((), ()))


def dot(a, b, dims):
    return lax.dot_general(a, b, dims, preferred_element_type=F32)


def toeplitz(row):
    x = jnp.broadcast_to(row, (8, LANES))
    x = pltpu.roll(x, LANES - (SEG - 1), axis=1)
    sub = lax.broadcasted_iota(jnp.int32, (8, LANES), 0)
    for bit in (1, 2, 4):
        x = jnp.where((sub & bit) != 0, pltpu.roll(x, bit, axis=1), x)
    rows = 8
    while rows < TILE:
        x = jnp.concatenate([x, pltpu.roll(x, rows, axis=1)], axis=0)
        rows *= 2
    return x


def skew_sum(z):
    rows = TILE
    while rows > 8:
        half = rows // 2
        z = z[:half] + pltpu.roll(z[half:], LANES - half, axis=1)
        rows = half
    for half in (4, 2, 1):
        z = z + pltpu.roll(pltpu.roll(z, 8 - half, axis=0), LANES - half, axis=1)
    return pltpu.roll(z, SEG - 1, axis=1)[0:1]


def partial_stats(s, dp):
    m = jnp.max(s, axis=0, keepdims=True)
    e = jnp.exp(s - m)
    return e, m, jnp.sum(e, axis=0, keepdims=True), jnp.sum(e * dp, axis=0, keepdims=True)


def merged(e, dp, mine, other):
    m, l, d = mine
    mo, lo, do = other
    top = jnp.maximum(m, mo)
    c, co = jnp.exp(m - top), jnp.exp(mo - top)
    inv = 1.0 / (l * c + lo * co)
    delta = (d * c + do * co) * inv
    p = e * (c * inv)
    return p, p * (dp - delta)


def pack(a, b):
    zero = jnp.zeros((2, TILE), F32)
    return jnp.concatenate([*a, *b, zero], axis=0)


def unpack(st):
    rows = [st[i : i + 1] for i in range(6)]
    return rows[:3], rows[3:]


def kernel(
    sp_n, tp_n, low_n, heads, tok,
    q_hbm, k_hbm, v_hbm, g_hbm, rb_ref,
    dq_all, dk_all, dv_all, bias_ref,
    q, k, v, g, rq, rg, rbp, table, gsum, acck, accv, es, dps,
    st_own, st_next, st_half, st_prev, dq_loc, dq_out, dq_in,
    b0, b1, b2, slots1, slots2, slots3,
    in_sem, q_s, q_r, g_s, g_r, so_s, so_r, sh_s, sh_r, dq_s, dq_r,
    e1_s, e1_r, e2_s, e2_r, e3_s, e3_r,
):
    sp = lax.axis_index("sp")
    dqo, dko, dvo = dq_all.at[0], dk_all.at[0], dv_all.at[0]
    tp = lax.axis_index("tp")
    high_n = sp_n // low_n
    low, high = lax.rem(sp, low_n), lax.div(sp, low_n)
    has_prev = sp > 0
    has_next = sp < sp_n - 1
    groups = tok // TILE
    lead = min(2, heads)
    half_heads = heads // 2
    step = 2 if heads % 2 == 0 else 1

    def cols_of(h):
        return pl.ds(pl.multiple_of(h * HEAD_DIM, HEAD_DIM), HEAD_DIM)

    loads = [
        pltpu.make_async_copy(src.at[0], dst, in_sem.at[i])
        for i, (src, dst) in enumerate(((q_hbm, q), (k_hbm, k), (g_hbm, g), (v_hbm, v)))
    ]
    for load in loads:
        load.start()

    barrier = pltpu.get_barrier_semaphore()

    def greet(axis, index):
        pl.semaphore_signal(barrier, inc=1, device_id={axis: index}, device_id_type=MESH)

    @pl.when(has_prev)
    def _():
        greet("sp", sp - 1)

    @pl.when(has_next)
    def _():
        greet("sp", sp + 1)

    for d in range(1, low_n):
        greet("sp", high * low_n + lax.rem(low + d, low_n))
    for d in range(1, high_n):
        greet("sp", lax.rem(high + d, high_n) * low_n + low)
    for d in range(1, tp_n):
        greet("tp", lax.rem(tp + d, tp_n))
    ends = (sp == 0).astype(jnp.int32) + (sp == sp_n - 1).astype(jnp.int32)
    pl.semaphore_wait(barrier, low_n + high_n + tp_n - 1 - ends)

    def q_copy(h):
        return pltpu.make_async_remote_copy(
            q_hbm.at[0, pl.ds(0, REACH), cols_of(h)], rq.at[h], q_s.at[h], q_r.at[h],
            device_id={"sp": sp - 1}, device_id_type=MESH)

    def g_copy(h):
        return pltpu.make_async_remote_copy(
            g_hbm.at[0, pl.ds(0, REACH), cols_of(h)], rg.at[h], g_s.at[h], g_r.at[h],
            device_id={"sp": sp - 1}, device_id_type=MESH)

    own_copy = pltpu.make_async_remote_copy(
        st_own, st_next, so_s.at[0], so_r.at[0], device_id={"sp": sp - 1}, device_id_type=MESH)

    def half_copy(h):
        return pltpu.make_async_remote_copy(
            st_half.at[h], st_prev.at[h], sh_s.at[h], sh_r.at[h],
            device_id={"sp": sp + 1}, device_id_type=MESH)

    def dq_copy(h):
        return pltpu.make_async_remote_copy(
            dq_out.at[h], dq_in.at[h], dq_s.at[h], dq_r.at[h],
            device_id={"sp": sp + 1}, device_id_type=MESH)

    @pl.when(has_prev)
    def _():
        @pl.loop(0, lead)
        def _(h):
            q_copy(h).start()
            g_copy(h).start()

    row_b = lax.broadcasted_iota(jnp.int32, (TILE, TILE), 0)
    col_r = lax.broadcasted_iota(jnp.int32, (TILE, TILE), 1)
    far_ok = (col_r < SEG) | (row_b >= SEG)
    diag_ok = (row_b < SEG) | (col_r >= SEG)
    beyond = col_r >= row_b
    lane = lax.broadcasted_iota(jnp.int32, (1, LANES), 1)

    rbp[...] = jnp.zeros_like(rbp)
    rbp[0:heads, 0:BUCKETS] = rb_ref[...]
    b0[...] = jnp.zeros_like(b0)

    for load in loads:
        load.wait()

    def tiles(h, group, keys_from, size, tab_part):
        cols = cols_of(h)
        rows = slice(group * TILE, (group + 1) * TILE)
        keys = slice(keys_from, keys_from + size)
        s = dot(k[keys, cols], q[rows, cols], NT) * SCALE + tab_part
        return s, dot(v[keys, cols], g[rows, cols], NT)

    def first_stats(h):
        row = rbp[pl.ds(h, 1), :]
        last = jnp.sum(jnp.where(lane == BUCKETS - 1, row, 0.0), axis=1, keepdims=True)
        both = toeplitz(row)
        diag = jnp.where(diag_ok, both[:, :TILE], LOW)
        table[h, 0:TILE] = jnp.where(far_ok, jnp.broadcast_to(last, (TILE, TILE)), LOW)
        table[h, TILE:REACH] = jnp.where(beyond, jnp.broadcast_to(last, (TILE, TILE)), both[:, TILE:])
        table[h, REACH:SPAN] = diag
        s, dp = tiles(h, 0, 0, TILE, diag)
        e0, *st0 = partial_stats(s, dp)
        es[h, 0:TILE] = e0
        dps[h, 0:TILE] = dp
        s, dp = tiles(h, 1, 0, REACH, table[h, TILE:SPAN])
        e1, *st1 = partial_stats(s, dp)
        es[h, TILE:SPAN] = e1
        dps[h, TILE:SPAN] = dp
        st_own[h] = pack(st0, st1)

    def whole_groups(h):
        cols = cols_of(h)
        for group in range(2, groups):
            start = (group - 2) * TILE
            rows = slice(group * TILE, (group + 1) * TILE)
            keys = slice(start, start + SPAN)
            s, dp = tiles(h, group, start, SPAN, table[h])
            e, m, l, d = partial_stats(s, dp)
            inv = 1.0 / l
            p = e * inv
            sg = p * (dp - d * inv)
            low_p = p.astype(BF16)
            low_g = (sg * SCALE).astype(BF16)
            part_k = dot(low_g, q[rows, cols], NN)
            part_v = dot(low_p, g[rows, cols], NN)
            if group == 2:
                gsum[h] = sg
                acck[h, 0:SPAN] = part_k
                accv[h, 0:SPAN] = part_v
            else:
                gsum[h] += sg
                old = slice(start, start + REACH)
                new = slice(start + REACH, start + SPAN)
                acck[h, old] += part_k[:REACH]
                accv[h, old] += part_v[:REACH]
                acck[h, new] = part_k[REACH:]
                accv[h, new] = part_v[REACH:]
            dqo[rows, cols] = dot(low_g, k[keys, cols], TN).astype(BF16)

    def each(body, ready=None):
        @pl.loop(0, heads // step)
        def _(i):
            several = [i * step + j for j in range(step)]
            if ready is not None:
                for h in several:
                    ready(h)
            for h in several:
                body(h)

    each(first_stats)

    @pl.when(has_prev)
    def _():
        own_copy.start()
        if lead < heads:
            @pl.loop(lead, heads)
            def _(h):
                q_copy(h).start()
                g_copy(h).start()

    @pl.when(jnp.logical_not(has_prev))
    def _():
        none = [jnp.full((1, TILE), LOW, F32), jnp.zeros((1, TILE), F32), jnp.zeros((1, TILE), F32)]
        nothing = pack(none, none)

        @pl.loop(0, heads)
        def _(h):
            st_prev[h] = nothing
            dq_in[h] = jnp.zeros((REACH, HEAD_DIM), BF16)

    each(whole_groups)

    @pl.when(has_next)
    def _():
        own_copy.wait_recv()

        def arrived(h):
            q_copy(h).wait_recv()
            g_copy(h).wait_recv()

        def halo(h):
            cols = cols_of(h)
            other0, other1 = unpack(st_next[h])

            def side(rows, keys_from, size, other):
                keys = slice(keys_from, keys_from + size)
                qr, gr = rq[h, rows], rg[h, rows]
                s = dot(k[keys, cols], qr, NT) * SCALE + table[h, 0:size]
                dp = dot(v[keys, cols], gr, NT)
                e, *mine = partial_stats(s, dp)
                p, sg = merged(e, dp, mine, other)
                gsum[h, 0:size] += sg
                low_p = p.astype(BF16)
                low_g = (sg * SCALE).astype(BF16)
                acck[h, keys] += dot(low_g, qr, NN)
                accv[h, keys] += dot(low_p, gr, NN)
                dq_out[h, rows] = dot(low_g, k[keys, cols], TN).astype(BF16)
                return mine

            mine0 = side(slice(0, TILE), tok - REACH, REACH, other0)
            mine1 = side(slice(TILE, REACH), tok - TILE, TILE, other1)
            st_half[h] = pack(mine0, mine1)
            half_copy(h).start()

        each(halo, arrived)

        @pl.loop(0, half_heads)
        def _(h):
            dq_copy(h).start()

    def merged_in(h):
        @pl.when(has_prev)
        def _():
            half_copy(h).wait_recv()

    def first_rows(h):
        cols = cols_of(h)
        other0, other1 = unpack(st_prev[h])
        mine0, mine1 = unpack(st_own[h])
        p0, sg0 = merged(es[h, 0:TILE], dps[h, 0:TILE], mine0, other0)
        p1, sg1 = merged(es[h, TILE:SPAN], dps[h, TILE:SPAN], mine1, other1)
        sums = gsum[h]
        far = sums[:TILE]
        mid = sums[TILE:REACH] + sg1[:TILE]
        diag = sums[REACH:] + sg1[TILE:] + sg0
        clipped = jnp.sum(far + jnp.where(beyond, mid, 0.0), axis=0, keepdims=True)
        clipped = jnp.sum(clipped, axis=1, keepdims=True)
        both = jnp.concatenate([diag, jnp.where(beyond, 0.0, mid)], axis=1)
        b0[pl.ds(h, 1), :] = skew_sum(both) + jnp.where(lane == BUCKETS - 1, clipped, 0.0)

        gl0, gl1 = (sg0 * SCALE).astype(BF16), (sg1 * SCALE).astype(BF16)
        q0, q1 = q[0:TILE, cols], q[TILE:REACH, cols]
        g0, g1 = g[0:TILE, cols], g[TILE:REACH, cols]
        for acc, out, a0, a1, x0, x1 in (
            (acck, dko, gl0, gl1, q0, q1), (accv, dvo, p0.astype(BF16), p1.astype(BF16), g0, g1)):
            second = dot(a1, x1, NN)
            out[0:TILE, cols] = (acc[h, 0:TILE] + second[:TILE] + dot(a0, x0, NN)).astype(BF16)
            out[TILE:REACH, cols] = (acc[h, TILE:REACH] + second[TILE:]).astype(BF16)
            out[REACH:tok, cols] = acc[h, REACH:tok].astype(BF16)
        dq_loc[h, 0:TILE] = dot(gl0, k[0:TILE, cols], TN)
        dq_loc[h, TILE:REACH] = dot(gl1, k[0:REACH, cols], TN)

    each(first_rows, merged_in)

    def copies(src, slots, send, recv, index, count, device):
        outgoing, incoming = [], []
        for d in range(1, count):
            peer = lax.rem(index + d, count)
            outgoing.append(pltpu.make_async_remote_copy(
                src, slots.at[index], send.at[d - 1], recv.at[index],
                device_id=device(peer), device_id_type=MESH))
            incoming.append(pltpu.make_async_remote_copy(
                src, slots.at[peer], send.at[d - 1], recv.at[peer],
                device_id=device(peer), device_id_type=MESH))
        return outgoing, incoming

    out1, in1 = copies(b0, slots1, e1_s, e1_r, high, high_n, lambda p: {"sp": p * low_n + low})
    out2, in2 = copies(b1, slots2, e2_s, e2_r, low, low_n, lambda p: {"sp": high * low_n + p})
    out3, in3 = copies(b2, slots3, e3_s, e3_r, tp, tp_n, lambda p: {"tp": p})

    for copy in out1:
        copy.start()
    slots1[high] = b0[...]

    for copy in in1:
        copy.wait_recv()
    total = slots1[0]
    for i in range(1, high_n):
        total += slots1[i]
    b1[...] = total
    for copy in out2:
        copy.start()
    slots2[low] = total

    @pl.when(has_next)
    def _():
        @pl.loop(half_heads, heads)
        def _(h):
            dq_copy(h).start()

    def finish(lo, hi):
        @pl.loop(lo, hi)
        def _(h):
            @pl.when(has_prev)
            def _():
                dq_copy(h).wait_recv()

            dqo[0:REACH, cols_of(h)] = (dq_loc[h] + dq_in[h].astype(F32)).astype(BF16)

    finish(0, half_heads)

    for copy in in2:
        copy.wait_recv()
    total = slots2[0]
    for i in range(1, low_n):
        total += slots2[i]
    b2[...] = total
    for copy in out3:
        copy.start()
    slots3[tp] = total

    finish(half_heads, heads)

    for copy in in3:
        copy.wait_recv()
    for i in range(tp_n):
        bias_ref[i * heads : (i + 1) * heads, :] = slots3[i, 0:heads, 0:BUCKETS]

    for copy in out1 + out2 + out3:
        copy.wait_send()

    @pl.when(has_prev)
    def _():
        own_copy.wait_send()

        @pl.loop(0, heads)
        def _(h):
            q_copy(h).wait_send()
            g_copy(h).wait_send()

    @pl.when(has_next)
    def _():
        @pl.loop(0, heads)
        def _(h):
            half_copy(h).wait_send()
            dq_copy(h).wait_send()


def local(sp_n, tp_n, queries, keys, values, rel_bias, out_grad):
    seq_count, tok, width = queries.shape
    heads = width // HEAD_DIM
    low_n = max(d for d in range(1, sp_n + 1) if sp_n % d == 0 and d * d <= sp_n)
    high_n = sp_n // low_n
    pad = -(-heads // 8) * 8
    any_spec = pl.BlockSpec(memory_space=pl.ANY)
    vmem_spec = pl.BlockSpec(memory_space=pltpu.VMEM)
    dma = pltpu.SemaphoreType.DMA
    big = pltpu.VMEM((tok, width), BF16)
    span = pltpu.VMEM((heads, SPAN, TILE), F32)
    acc = pltpu.VMEM((heads, tok, HEAD_DIM), F32)
    stats = pltpu.VMEM((heads, 8, TILE), F32)
    halo = pltpu.VMEM((heads, REACH, HEAD_DIM), BF16)
    row = pltpu.VMEM((pad, LANES), F32)
    return pl.pallas_call(
        functools.partial(kernel, sp_n, tp_n, low_n, heads, tok),
        out_shape=(pltpu.VMEM(queries.shape, BF16),) * 3 + ( jax.ShapeDtypeStruct((heads * tp_n, BUCKETS), F32),),
        in_specs=[any_spec] * 4 + [vmem_spec],
        out_specs=(vmem_spec,) * 4,
        scratch_shapes=[big] * 4 + [halo, halo, row, span, span, acc, acc, span, span]
        + [stats] * 4
        + [pltpu.VMEM((heads, REACH, HEAD_DIM), F32), halo, halo]
        + [row, row, row]
        + [pltpu.VMEM((n, pad, LANES), F32) for n in (high_n, low_n, tp_n)]
        + [dma((4,))] + [dma((heads,))] * 4 + [dma((1,))] * 2 + [dma((heads,))] * 4
        + [dma((high_n,))] * 2 + [dma((low_n,))] * 2 + [dma((tp_n,))] * 2,
        compiler_params=pltpu.CompilerParams(
            collective_id=0, has_side_effects=True, vmem_limit_bytes=64_500_000
        ),
    )(queries, keys, values, out_grad, rel_bias)


def solution(mesh):
    split = P(None, "sp", "tp")
    return jax.shard_map(
        functools.partial(local, mesh.shape["sp"], mesh.shape["tp"]),
        mesh=mesh,
        in_specs=(split, split, split, P("tp", None), split),
        out_specs=(split, split, split, P()),
        check_vma=False,
    )
```

```python
import functools

import jax
import jax.numpy as jnp
from jax import lax
from jax.experimental import pallas as pl
from jax.experimental.pallas import tpu as pltpu
from jax.sharding import PartitionSpec as P

HEAD_DIM = 128
SEG = 64
LEFT = 4
BUCKETS = 192
TILE = 2 * SEG
REACH = LEFT * SEG
SPAN = REACH + TILE
LANES = 256
LOW = -1e30
SCALE = HEAD_DIM ** (-0.5)
MESH = pl.DeviceIdType.MESH
F32 = jnp.float32
BF16 = jnp.bfloat16

NT = (((1,), (1,)), ((), ()))
TN = (((0,), (0,)), ((), ()))
NN = (((1,), (0,)), ((), ()))


def dot(a, b, dims):
    return lax.dot_general(a, b, dims, preferred_element_type=F32)


def toeplitz(row):
    x = jnp.broadcast_to(row, (8, LANES))
    x = pltpu.roll(x, LANES - (SEG - 1), axis=1)
    sub = lax.broadcasted_iota(jnp.int32, (8, LANES), 0)
    for bit in (1, 2, 4):
        x = jnp.where((sub & bit) != 0, pltpu.roll(x, bit, axis=1), x)
    rows = 8
    while rows < TILE:
        x = jnp.concatenate([x, pltpu.roll(x, rows, axis=1)], axis=0)
        rows *= 2
    return x


def skew_sum(z):
    rows = TILE
    while rows > 8:
        half = rows // 2
        z = z[:half] + pltpu.roll(z[half:], LANES - half, axis=1)
        rows = half
    for half in (4, 2, 1):
        z = z + pltpu.roll(pltpu.roll(z, 8 - half, axis=0), LANES - half, axis=1)
    return pltpu.roll(z, SEG - 1, axis=1)[0:1]


def partial_stats(s, dp):
    m = jnp.max(s, axis=0, keepdims=True)
    e = jnp.exp(s - m)
    return e, m, jnp.sum(e, axis=0, keepdims=True), jnp.sum(e * dp, axis=0, keepdims=True)


def merged(e, dp, mine, other):
    m, l, d = mine
    mo, lo, do = other
    top = jnp.maximum(m, mo)
    c, co = jnp.exp(m - top), jnp.exp(mo - top)
    inv = 1.0 / (l * c + lo * co)
    delta = (d * c + do * co) * inv
    p = e * (c * inv)
    return p, p * (dp - delta)


def pack(a, b):
    zero = jnp.zeros((2, TILE), F32)
    return jnp.concatenate([*a, *b, zero], axis=0)


def unpack(st):
    rows = [st[i : i + 1] for i in range(6)]
    return rows[:3], rows[3:]


def kernel(
    sp_n, tp_n, low_n, heads, tok,
    q_hbm, k_hbm, v_hbm, g_hbm, rb_ref,
    dq_all, dk_all, dv_all, bias_ref,
    q, k, v, g, rq, rg, rbp, table, gsum, acck, accv, es, dps,
    st_own, st_next, st_half, st_prev, dq_loc, dq_out, dq_in,
    b0, b1, b2, slots1, slots2, slots3,
    in_sem, q_s, q_r, g_s, g_r, so_s, so_r, sh_s, sh_r, dq_s, dq_r,
    e1_s, e1_r, e2_s, e2_r, e3_s, e3_r,
):
    sp = lax.axis_index("sp")
    dqo, dko, dvo = dq_all.at[0], dk_all.at[0], dv_all.at[0]
    tp = lax.axis_index("tp")
    high_n = sp_n // low_n
    low, high = lax.rem(sp, low_n), lax.div(sp, low_n)
    has_prev = sp > 0
    has_next = sp < sp_n - 1
    groups = tok // TILE
    lead = min(2, heads)
    half_heads = heads // 2
    step = 2 if heads % 2 == 0 else 1

    def cols_of(h):
        return pl.ds(pl.multiple_of(h * HEAD_DIM, HEAD_DIM), HEAD_DIM)

    loads = [
        pltpu.make_async_copy(src.at[0], dst, in_sem.at[i])
        for i, (src, dst) in enumerate(((q_hbm, q), (k_hbm, k), (g_hbm, g), (v_hbm, v)))
    ]
    for load in loads:
        load.start()

    barrier = pltpu.get_barrier_semaphore()

    def greet(axis, index):
        pl.semaphore_signal(barrier, inc=1, device_id={axis: index}, device_id_type=MESH)

    @pl.when(has_prev)
    def _():
        greet("sp", sp - 1)

    @pl.when(has_next)
    def _():
        greet("sp", sp + 1)

    for d in range(1, low_n):
        greet("sp", high * low_n + lax.rem(low + d, low_n))
    for d in range(1, high_n):
        greet("sp", lax.rem(high + d, high_n) * low_n + low)
    for d in range(1, tp_n):
        greet("tp", lax.rem(tp + d, tp_n))
    ends = (sp == 0).astype(jnp.int32) + (sp == sp_n - 1).astype(jnp.int32)
    pl.semaphore_wait(barrier, low_n + high_n + tp_n - 1 - ends)

    def q_copy(h):
        return pltpu.make_async_remote_copy(
            q_hbm.at[0, pl.ds(0, REACH), cols_of(h)], rq.at[h], q_s.at[h], q_r.at[h],
            device_id={"sp": sp - 1}, device_id_type=MESH)

    def g_copy(h):
        return pltpu.make_async_remote_copy(
            g_hbm.at[0, pl.ds(0, REACH), cols_of(h)], rg.at[h], g_s.at[h], g_r.at[h],
            device_id={"sp": sp - 1}, device_id_type=MESH)

    own_copy = pltpu.make_async_remote_copy(
        st_own, st_next, so_s.at[0], so_r.at[0], device_id={"sp": sp - 1}, device_id_type=MESH)

    def half_copy(h):
        return pltpu.make_async_remote_copy(
            st_half.at[h], st_prev.at[h], sh_s.at[h], sh_r.at[h],
            device_id={"sp": sp + 1}, device_id_type=MESH)

    def dq_copy(h):
        return pltpu.make_async_remote_copy(
            dq_out.at[h], dq_in.at[h], dq_s.at[h], dq_r.at[h],
            device_id={"sp": sp + 1}, device_id_type=MESH)

    @pl.when(has_prev)
    def _():
        @pl.loop(0, lead)
        def _(h):
            q_copy(h).start()
            g_copy(h).start()

    row_b = lax.broadcasted_iota(jnp.int32, (TILE, TILE), 0)
    col_r = lax.broadcasted_iota(jnp.int32, (TILE, TILE), 1)
    far_ok = (col_r < SEG) | (row_b >= SEG)
    diag_ok = (row_b < SEG) | (col_r >= SEG)
    beyond = col_r >= row_b
    lane = lax.broadcasted_iota(jnp.int32, (1, LANES), 1)

    rbp[...] = jnp.zeros_like(rbp)
    rbp[0:heads, 0:BUCKETS] = rb_ref[...]
    b0[...] = jnp.zeros_like(b0)

    for load in loads:
        load.wait()

    def tiles(h, group, keys_from, size, tab_part):
        cols = cols_of(h)
        rows = slice(group * TILE, (group + 1) * TILE)
        keys = slice(keys_from, keys_from + size)
        s = dot(k[keys, cols], q[rows, cols], NT) * SCALE + tab_part
        return s, dot(v[keys, cols], g[rows, cols], NT)

    def first_stats(h):
        row = rbp[pl.ds(h, 1), :]
        last = jnp.sum(jnp.where(lane == BUCKETS - 1, row, 0.0), axis=1, keepdims=True)
        both = toeplitz(row)
        diag = jnp.where(diag_ok, both[:, :TILE], LOW)
        table[h, 0:TILE] = jnp.where(far_ok, jnp.broadcast_to(last, (TILE, TILE)), LOW)
        table[h, TILE:REACH] = jnp.where(beyond, jnp.broadcast_to(last, (TILE, TILE)), both[:, TILE:])
        table[h, REACH:SPAN] = diag
        s, dp = tiles(h, 0, 0, TILE, diag)
        e0, *st0 = partial_stats(s, dp)
        es[h, 0:TILE] = e0
        dps[h, 0:TILE] = dp
        s, dp = tiles(h, 1, 0, REACH, table[h, TILE:SPAN])
        e1, *st1 = partial_stats(s, dp)
        es[h, TILE:SPAN] = e1
        dps[h, TILE:SPAN] = dp
        st_own[h] = pack(st0, st1)

    def whole_groups(h):
        cols = cols_of(h)
        for group in range(2, groups):
            start = (group - 2) * TILE
            rows = slice(group * TILE, (group + 1) * TILE)
            keys = slice(start, start + SPAN)
            s, dp = tiles(h, group, start, SPAN, table[h])
            e, m, l, d = partial_stats(s, dp)
            inv = 1.0 / l
            p = e * inv
            sg = p * (dp - d * inv)
            low_p = p.astype(BF16)
            low_g = (sg * SCALE).astype(BF16)
            part_k = dot(low_g, q[rows, cols], NN)
            part_v = dot(low_p, g[rows, cols], NN)
            if group == 2:
                gsum[h] = sg
                acck[h, 0:SPAN] = part_k
                accv[h, 0:SPAN] = part_v
            else:
                gsum[h] += sg
                old = slice(start, start + REACH)
                new = slice(start + REACH, start + SPAN)
                acck[h, old] += part_k[:REACH]
                accv[h, old] += part_v[:REACH]
                acck[h, new] = part_k[REACH:]
                accv[h, new] = part_v[REACH:]
            dqo[rows, cols] = dot(low_g, k[keys, cols], TN).astype(BF16)

    def each(body, ready=None):
        @pl.loop(0, heads // step)
        def _(i):
            several = [i * step + j for j in range(step)]
            if ready is not None:
                for h in several:
                    ready(h)
            for h in several:
                body(h)

    each(first_stats)

    @pl.when(has_prev)
    def _():
        own_copy.start()
        if lead < heads:
            @pl.loop(lead, heads)
            def _(h):
                q_copy(h).start()
                g_copy(h).start()

    @pl.when(jnp.logical_not(has_prev))
    def _():
        none = [jnp.full((1, TILE), LOW, F32), jnp.zeros((1, TILE), F32), jnp.zeros((1, TILE), F32)]
        nothing = pack(none, none)

        @pl.loop(0, heads)
        def _(h):
            st_prev[h] = nothing
            dq_in[h] = jnp.zeros((REACH, HEAD_DIM), BF16)

    each(whole_groups)

    @pl.when(has_next)
    def _():
        own_copy.wait_recv()

        def arrived(h):
            q_copy(h).wait_recv()
            g_copy(h).wait_recv()

        def halo(h):
            cols = cols_of(h)
            other0, other1 = unpack(st_next[h])

            def side(rows, keys_from, size, other):
                keys = slice(keys_from, keys_from + size)
                qr, gr = rq[h, rows], rg[h, rows]
                s = dot(k[keys, cols], qr, NT) * SCALE + table[h, 0:size]
                dp = dot(v[keys, cols], gr, NT)
                e, *mine = partial_stats(s, dp)
                p, sg = merged(e, dp, mine, other)
                gsum[h, 0:size] += sg
                low_p = p.astype(BF16)
                low_g = (sg * SCALE).astype(BF16)
                acck[h, keys] += dot(low_g, qr, NN)
                accv[h, keys] += dot(low_p, gr, NN)
                dq_out[h, rows] = dot(low_g, k[keys, cols], TN).astype(BF16)
                return mine

            mine0 = side(slice(0, TILE), tok - REACH, REACH, other0)
            mine1 = side(slice(TILE, REACH), tok - TILE, TILE, other1)
            st_half[h] = pack(mine0, mine1)
            half_copy(h).start()

        each(halo, arrived)

        @pl.loop(0, half_heads)
        def _(h):
            dq_copy(h).start()

    def merged_in(h):
        @pl.when(has_prev)
        def _():
            half_copy(h).wait_recv()

    def first_rows(h):
        cols = cols_of(h)
        other0, other1 = unpack(st_prev[h])
        mine0, mine1 = unpack(st_own[h])
        p0, sg0 = merged(es[h, 0:TILE], dps[h, 0:TILE], mine0, other0)
        p1, sg1 = merged(es[h, TILE:SPAN], dps[h, TILE:SPAN], mine1, other1)
        sums = gsum[h]
        far = sums[:TILE]
        mid = sums[TILE:REACH] + sg1[:TILE]
        diag = sums[REACH:] + sg1[TILE:] + sg0
        clipped = jnp.sum(far + jnp.where(beyond, mid, 0.0), axis=0, keepdims=True)
        clipped = jnp.sum(clipped, axis=1, keepdims=True)
        both = jnp.concatenate([diag, jnp.where(beyond, 0.0, mid)], axis=1)
        b0[pl.ds(h, 1), :] = skew_sum(both) + jnp.where(lane == BUCKETS - 1, clipped, 0.0)

        gl0, gl1 = (sg0 * SCALE).astype(BF16), (sg1 * SCALE).astype(BF16)
        q0, q1 = q[0:TILE, cols], q[TILE:REACH, cols]
        g0, g1 = g[0:TILE, cols], g[TILE:REACH, cols]
        for acc, out, a0, a1, x0, x1 in (
            (acck, dko, gl0, gl1, q0, q1), (accv, dvo, p0.astype(BF16), p1.astype(BF16), g0, g1)):
            second = dot(a1, x1, NN)
            out[0:TILE, cols] = (acc[h, 0:TILE] + second[:TILE] + dot(a0, x0, NN)).astype(BF16)
            out[TILE:REACH, cols] = (acc[h, TILE:REACH] + second[TILE:]).astype(BF16)
            out[REACH:tok, cols] = acc[h, REACH:tok].astype(BF16)
        dq_loc[h, 0:TILE] = dot(gl0, k[0:TILE, cols], TN)
        dq_loc[h, TILE:REACH] = dot(gl1, k[0:REACH, cols], TN)

    each(first_rows, merged_in)

    def copies(src, slots, send, recv, index, count, device):
        outgoing, incoming = [], []
        for d in range(1, count):
            peer = lax.rem(index + d, count)
            outgoing.append(pltpu.make_async_remote_copy(
                src, slots.at[index], send.at[d - 1], recv.at[index],
                device_id=device(peer), device_id_type=MESH))
            incoming.append(pltpu.make_async_remote_copy(
                src, slots.at[peer], send.at[d - 1], recv.at[peer],
                device_id=device(peer), device_id_type=MESH))
        return outgoing, incoming

    out1, in1 = copies(b0, slots1, e1_s, e1_r, high, high_n, lambda p: {"sp": p * low_n + low})
    out2, in2 = copies(b1, slots2, e2_s, e2_r, low, low_n, lambda p: {"sp": high * low_n + p})
    out3, in3 = copies(b2, slots3, e3_s, e3_r, tp, tp_n, lambda p: {"tp": p})

    for copy in out1:
        copy.start()
    slots1[high] = b0[...]

    for copy in in1:
        copy.wait_recv()
    total = slots1[0]
    for i in range(1, high_n):
        total += slots1[i]
    b1[...] = total
    for copy in out2:
        copy.start()
    slots2[low] = total

    @pl.when(has_next)
    def _():
        @pl.loop(half_heads, heads)
        def _(h):
            dq_copy(h).start()

    def finish(lo, hi):
        @pl.loop(lo, hi)
        def _(h):
            @pl.when(has_prev)
            def _():
                dq_copy(h).wait_recv()

            dqo[0:REACH, cols_of(h)] = (dq_loc[h] + dq_in[h].astype(F32)).astype(BF16)

    finish(0, half_heads)

    for copy in in2:
        copy.wait_recv()
    total = slots2[0]
    for i in range(1, low_n):
        total += slots2[i]
    b2[...] = total
    for copy in out3:
        copy.start()
    slots3[tp] = total

    finish(half_heads, heads)

    for copy in in3:
        copy.wait_recv()
    for i in range(tp_n):
        bias_ref[i * heads : (i + 1) * heads, :] = slots3[i, 0:heads, 0:BUCKETS]

    for copy in out1 + out2 + out3:
        copy.wait_send()

    @pl.when(has_prev)
    def _():
        own_copy.wait_send()

        @pl.loop(0, heads)
        def _(h):
            q_copy(h).wait_send()
            g_copy(h).wait_send()

    @pl.when(has_next)
    def _():
        @pl.loop(0, heads)
        def _(h):
            half_copy(h).wait_send()
            dq_copy(h).wait_send()


def store(*refs):
    sem = refs[-1]
    copies = [pltpu.make_async_copy(refs[i], refs[4 + i], sem.at[i]) for i in range(4)]
    for copy in copies:
        copy.start()
    for copy in copies:
        copy.wait()


def local(sp_n, tp_n, queries, keys, values, rel_bias, out_grad):
    seq_count, tok, width = queries.shape
    heads = width // HEAD_DIM
    low_n = max(d for d in range(1, sp_n + 1) if sp_n % d == 0 and d * d <= sp_n)
    high_n = sp_n // low_n
    pad = -(-heads // 8) * 8
    any_spec = pl.BlockSpec(memory_space=pl.ANY)
    vmem_spec = pl.BlockSpec(memory_space=pltpu.VMEM)
    dma = pltpu.SemaphoreType.DMA
    big = pltpu.VMEM((tok, width), BF16)
    span = pltpu.VMEM((heads, SPAN, TILE), F32)
    acc = pltpu.VMEM((heads, tok, HEAD_DIM), F32)
    stats = pltpu.VMEM((heads, 8, TILE), F32)
    halo = pltpu.VMEM((heads, REACH, HEAD_DIM), BF16)
    row = pltpu.VMEM((pad, LANES), F32)
    held = pl.pallas_call(
        functools.partial(kernel, sp_n, tp_n, low_n, heads, tok),
        out_shape=(pltpu.VMEM(queries.shape, BF16),) * 3
        + (pltpu.VMEM((heads * tp_n, BUCKETS), F32),),
        in_specs=[any_spec] * 4 + [vmem_spec],
        out_specs=(vmem_spec,) * 4,
        scratch_shapes=[big] * 4 + [halo, halo, row, span, span, acc, acc, span, span]
        + [stats] * 4
        + [pltpu.VMEM((heads, REACH, HEAD_DIM), F32), halo, halo]
        + [row, row, row]
        + [pltpu.VMEM((n, pad, LANES), F32) for n in (high_n, low_n, tp_n)]
        + [dma((4,))] + [dma((heads,))] * 4 + [dma((1,))] * 2 + [dma((heads,))] * 4
        + [dma((high_n,))] * 2 + [dma((low_n,))] * 2 + [dma((tp_n,))] * 2,
        compiler_params=pltpu.CompilerParams(
            collective_id=0, has_side_effects=True, vmem_limit_bytes=64_500_000
        ),
    )(queries, keys, values, out_grad, rel_bias)
    return pl.pallas_call(
        store,
        out_shape=tuple(jax.ShapeDtypeStruct(x.shape, x.dtype) for x in held),
        in_specs=[any_spec] * 4,
        out_specs=(any_spec,) * 4,
        scratch_shapes=[dma((4,))],
        compiler_params=pltpu.CompilerParams(vmem_limit_bytes=1024 * 1024),
    )(*held)


def solution(mesh):
    split = P(None, "sp", "tp")
    return jax.shard_map(
        functools.partial(local, mesh.shape["sp"], mesh.shape["tp"]),
        mesh=mesh,
        in_specs=(split, split, split, P("tp", None), split),
        out_specs=(split, split, split, P()),
        check_vma=False,
    )
```
